32 devices in a mesh: sp: 8 (over z, y), tp: 4 (over x, core).
Axes of the slice: x: 2, y: 2, z: 4, core: 2. Of those that a mesh axis runs over, the one named last changes fastest.
Arguments:
- inputs: bfloat16 [4096, 4096], P(('sp', 'tp')), may hold values from -42 to 42
- a_query_w: bfloat16 [4096, 2048], P(None, 'tp'), may hold values from -0.12570312 to 0.12570312
- a_key_w: bfloat16 [4096, 2048], P(None, 'tp'), may hold values from -0.12570312 to 0.12570312
- a_value_w: bfloat16 [4096, 2048], P(None, 'tp'), may hold values from -0.09375 to 0.09375
- b_query_w: bfloat16 [4096, 2048], P(None, 'tp'), may hold values from -0.12570312 to 0.12570312
- b_key_w: bfloat16 [4096, 512], P(None, 'tp'), may hold values from -0.12570312 to 0.12570312
- b_value_w: bfloat16 [4096, 512], P(None, 'tp'), may hold values from -0.09375 to 0.09375
- head_lambda: float32 [16], P('tp'), may hold values from 0.3 to 0.8
- head_gain: float32 [128], replicated, may hold values from 0.1 to 1.9
- sink_logit: float32 [32], P('tp'), may hold values from 2 to 7
- a_out_w: bfloat16 [2048, 4096], P('tp'), may hold values from -0.125 to 0.125
- b_out_w: bfloat16 [2048, 4096], P('tp'), may hold values from -0.625 to 0.625
Outputs:
- mixed: bfloat16 [4096, 4096], P(('sp', 'tp'))
The draws below stay inside these ranges and needn't reach their ends.
All inputs are finite; a program needn't handle non-finite values.
Results may differ from the reference program's by a relative error of at most 0.015.
Values may be sent and summed in bfloat16 or wider, within the bound.
No kernel may reach another device: no remote copies, remote signals or barrier semaphores. Data moves between devices by JAX's collectives and lax.ppermute only.
A program may use at most 128 MiB of HBM per device.

```python
import math
import jax
import jax.numpy as jnp
from jax import lax

D = 4096
A_HEADS = 16
B_HEADS = 32
KV_HEADS = 8
HEAD_DIM = 64
VALUE_DIM = 128
WINDOW = 128
TOKENS = 4096
N_TP = 4


def plain_noise(key, salt, columns):
    values = jnp.clip(jax.random.normal(jax.random.fold_in(key, salt), (D, columns), jnp.float32), -6.0, 6.0)
    return values * (1.32 * D ** (-0.5))


def draw_inputs(key, part):
    values = jnp.clip(jax.random.normal(jax.random.fold_in(key, 10), (TOKENS, D), jnp.float32), -6.0, 6.0)
    return values.astype(jnp.bfloat16)


def draw_a_query_w(key, part):
    columns = 2 * A_HEADS * HEAD_DIM
    values = plain_noise(key, 11, columns)
    return values.astype(jnp.bfloat16)


def draw_a_key_w(key, part):
    columns = 2 * A_HEADS * HEAD_DIM
    values = plain_noise(key, 12, columns)
    return values.astype(jnp.bfloat16)


def draw_b_query_w(key, part):
    columns = B_HEADS * HEAD_DIM
    values = plain_noise(key, 13, columns)
    return values.astype(jnp.bfloat16)


def draw_b_key_w(key, part):
    columns = KV_HEADS * HEAD_DIM
    values = plain_noise(key, 14, columns)
    return values.astype(jnp.bfloat16)


def block_levels(key, shape, shards, smallest, high):
    gain, own = 1.0, jax.random.fold_in(key, 6)
    for axis_at, shards_of in shards:
        steps = jnp.exp(jax.random.uniform(jax.random.fold_in(own, axis_at), (shards_of,), jnp.float32, smallest / len(shards), high / len(shards)))
        gain = gain * jnp.repeat(steps, shape[axis_at] // shards_of).reshape([-1 if axis == axis_at else 1 for axis in range(len(shape))])
    return gain


def normal_values(own_key, extent, width, reach, cuts=(), kind=jnp.bfloat16):
    level = block_levels(own_key, extent, cuts, -0.22, 0.18) if cuts else 1.0
    drawn = jax.random.normal(own_key, extent, jnp.float32) * width * level
    return jnp.minimum(jnp.maximum(drawn, -reach), reach).astype(kind)


def setup_inputs(seed: int = 0) -> dict:
    seeds = jax.random.split(jax.random.key(seed), 13)
    inputs = draw_inputs(jax.random.fold_in(seeds[12], 71), 0)
    a_query_w = draw_a_query_w(jax.random.fold_in(seeds[12], 71), 0)
    a_key_w = draw_a_key_w(jax.random.fold_in(seeds[12], 71), 0)
    a_value_w = normal_values(seeds[3], (D, A_HEADS * VALUE_DIM), D ** -0.5, 0.09375, ((1, 4),))
    b_query_w = draw_b_query_w(jax.random.fold_in(seeds[12], 71), 0)
    b_key_w = draw_b_key_w(jax.random.fold_in(seeds[12], 71), 0)
    b_value_w = normal_values(seeds[6], (D, KV_HEADS * HEAD_DIM), D ** -0.5, 0.09375, ((1, 4),))
    head_lambda = jnp.clip(0.3 + 0.5 * jax.random.uniform(seeds[7], (A_HEADS,), jnp.float32) ** block_levels(seeds[7], (A_HEADS,), ((0, 4),), -0.2, 0.2), 0.3, 0.8)
    head_gain = jnp.clip(1.0 + 0.18 * jax.random.normal(seeds[8], (VALUE_DIM,), jnp.float32), 0.1, 1.9)
    sink_logit = jnp.clip(2.0 + 5.0 * jax.random.uniform(seeds[9], (B_HEADS,), jnp.float32) ** block_levels(seeds[9], (B_HEADS,), ((0, 4),), -0.2, 0.2), 2.0, 7.0)
    a_out_w = normal_values(seeds[10], (A_HEADS * VALUE_DIM, D), (A_HEADS * VALUE_DIM) ** -0.5, 0.125, ((0, 4),))
    b_out_w = normal_values(seeds[11], (B_HEADS * HEAD_DIM, D), (5.0 * (B_HEADS * HEAD_DIM) ** -0.5), 0.625, ((0, 4),))
    return {"inputs": inputs, "a_query_w": a_query_w, "a_key_w": a_key_w, "a_value_w": a_value_w, "b_query_w": b_query_w, "b_key_w": b_key_w, "b_value_w": b_value_w, "head_lambda": head_lambda, "head_gain": head_gain, "sink_logit": sink_logit, "a_out_w": a_out_w, "b_out_w": b_out_w}


norm_eps = 0.0001
head_scale = 0.8
mask_fill = -1e+30

def rounded(value):
    return lax.optimization_barrier(value.astype(jnp.bfloat16)).astype(jnp.float32)

def reference(inputs, a_query_w, a_key_w, a_value_w, b_query_w, b_key_w, b_value_w, head_lambda, head_gain, sink_logit, a_out_w, b_out_w):
    length = inputs.shape[0]
    group_size = B_HEADS // KV_HEADS
    score_scale = HEAD_DIM ** (-0.5)
    a_query = jnp.dot(inputs, a_query_w, preferred_element_type=jnp.float32).astype(jnp.bfloat16).reshape(length, A_HEADS, 2, HEAD_DIM)
    a_key = jnp.dot(inputs, a_key_w, preferred_element_type=jnp.float32).astype(jnp.bfloat16).reshape(length, A_HEADS, 2, HEAD_DIM)
    a_value = jnp.dot(inputs, a_value_w, preferred_element_type=jnp.float32).astype(jnp.bfloat16).reshape(length, A_HEADS, VALUE_DIM)
    b_query = jnp.dot(inputs, b_query_w, preferred_element_type=jnp.float32).astype(jnp.bfloat16).reshape(length, KV_HEADS, group_size, HEAD_DIM)
    b_key = jnp.dot(inputs, b_key_w, preferred_element_type=jnp.float32).astype(jnp.bfloat16).reshape(length, KV_HEADS, HEAD_DIM)
    b_value = jnp.dot(inputs, b_value_w, preferred_element_type=jnp.float32).astype(jnp.bfloat16).reshape(length, KV_HEADS, HEAD_DIM)
    query_span = math.gcd(length, 128)
    span_count = length // query_span
    key_pos = jnp.arange(length, dtype=jnp.int32)
    keys_wide = a_key.astype(jnp.float32)
    values_wide = a_value.astype(jnp.float32)

    def differential(block_index):
        block_start = block_index * query_span
        queries = lax.dynamic_slice_in_dim(a_query, block_start, query_span, 0).astype(jnp.float32)
        scores = jnp.einsum('qhmd,khmd->hmqk', queries, keys_wide) * score_scale
        query_pos = block_start + jnp.arange(query_span, dtype=jnp.int32)
        allowed = query_pos[:, None] >= key_pos[None, :]
        scores = jnp.where(allowed, scores, mask_fill)
        row_top = lax.optimization_barrier(jnp.max(scores, axis=-1, keepdims=True))
        weights = jnp.where(allowed, jnp.exp(scores - row_top), 0.0)
        row_total = lax.optimization_barrier(jnp.sum(weights, axis=-1))
        means = jnp.einsum('hmqk,khe->hmqe', rounded(weights), values_wide) / row_total[..., None]
        difference = means[:, 0] - head_lambda[:, None, None] * means[:, 1]
        mean_square = lax.optimization_barrier(jnp.mean(difference * difference, axis=-1, keepdims=True))
        return (difference * lax.rsqrt(mean_square + norm_eps) * head_gain * head_scale).astype(jnp.bfloat16)
    a_heads = lax.map(differential, jnp.arange(span_count, dtype=jnp.int32))
    a_heads = jnp.transpose(a_heads, (1, 0, 2, 3)).reshape(A_HEADS, length, VALUE_DIM)
    pad_keys = jnp.concatenate([jnp.zeros((WINDOW, KV_HEADS, HEAD_DIM), jnp.bfloat16), b_key], axis=0).astype(jnp.float32)
    pad_values = jnp.concatenate([jnp.zeros((WINDOW, KV_HEADS, HEAD_DIM), jnp.bfloat16), b_value], axis=0).astype(jnp.float32)
    sink_term = sink_logit.reshape(KV_HEADS, group_size)[:, :, None]

    def windowed(block_index):
        block_start = block_index * query_span
        queries = lax.dynamic_slice_in_dim(b_query, block_start, query_span, 0).astype(jnp.float32)
        block_keys = lax.dynamic_slice_in_dim(pad_keys, block_start, query_span + WINDOW, 0)
        block_values = lax.dynamic_slice_in_dim(pad_values, block_start, query_span + WINDOW, 0)
        scores = jnp.einsum('qhgd,khd->hgqk', queries, block_keys) * score_scale
        query_pos = block_start + jnp.arange(query_span, dtype=jnp.int32)
        near_pos = block_start - WINDOW + jnp.arange(query_span + WINDOW, dtype=jnp.int32)
        distance = query_pos[:, None] - near_pos[None, :]
        allowed = (distance >= 0) & (distance < WINDOW) & (near_pos[None, :] >= 0)
        scores = jnp.where(allowed, scores, mask_fill)
        row_top = jnp.maximum(lax.optimization_barrier(jnp.max(scores, axis=-1)), sink_term)
        weights = jnp.where(allowed, jnp.exp(scores - row_top[..., None]), 0.0)
        row_total = lax.optimization_barrier(jnp.sum(weights, axis=-1)) + jnp.exp(sink_term - row_top)
        probs = weights / row_total[..., None]
        block_out = jnp.einsum('hgqk,khd->qhgd', rounded(probs), block_values)
        return block_out.reshape(query_span, B_HEADS * HEAD_DIM).astype(jnp.bfloat16)
    b_heads = lax.map(windowed, jnp.arange(span_count, dtype=jnp.int32)).reshape(length, B_HEADS * HEAD_DIM)
    heads_local = A_HEADS // N_TP
    cols_local = B_HEADS * HEAD_DIM // N_TP
    summed = jnp.zeros((length, D), jnp.float32)
    for group_index in range(N_TP):
        a_part = a_heads[group_index * heads_local:(group_index + 1) * heads_local].astype(jnp.float32)
        a_weight = a_out_w[group_index * heads_local * VALUE_DIM:(group_index + 1) * heads_local * VALUE_DIM]
        a_weight = a_weight.reshape(heads_local, VALUE_DIM, D).astype(jnp.float32)
        b_part = b_heads[:, group_index * cols_local:(group_index + 1) * cols_local]
        b_weight = b_out_w[group_index * cols_local:(group_index + 1) * cols_local]
        partial_sum = jnp.einsum('hqe,hen->qn', a_part, a_weight) + jnp.dot(b_part, b_weight, preferred_element_type=jnp.float32)
        summed = summed + rounded(partial_sum)
    return summed.astype(jnp.bfloat16)
```

```python
import functools
import math

import jax
import jax.numpy as jnp
from jax import lax
from jax.experimental import pallas as pl
from jax.experimental.pallas import tpu as pltpu
from jax.sharding import PartitionSpec as P

HEAD_DIM = 64
VALUE_DIM = 128
WINDOW = 128

norm_eps = 0.0001
head_scale = 0.8
mask_fill = -1e30


F32 = jnp.float32
BF16 = jnp.bfloat16
ANY = pl.BlockSpec(memory_space=pl.ANY)
SMEM = pl.BlockSpec(memory_space=pltpu.SMEM)
VMEM = pl.BlockSpec(memory_space=pltpu.VMEM)
VMEM_LIMIT = 56 * 1024 * 1024


def swap(value, axis, by):
    size = lax.axis_size(axis)
    return lax.ppermute(value, axis, [(i, i ^ by) for i in range(size)])


def params():
    return pltpu.CompilerParams(vmem_limit_bytes=VMEM_LIMIT)


def run_copies(copies):
    for copy in copies:
        copy.start()
    return copies


def project_a(chunks, weights, place, slots):
    rows, depth = chunks[0].shape
    group = rows * len(chunks)
    width = VALUE_DIM

    def kernel(place_ref, *refs):
        x_refs = refs[: len(chunks)]
        w_refs = refs[len(chunks) : len(chunks) + 3]
        outs = refs[len(chunks) + 3 : len(chunks) + 3 + slots]
        x_buf, w_buf, x_sem, w_sem = refs[len(chunks) + 3 + slots :]
        core = place_ref[2] % 2
        hz = place_ref[0]
        x_copies = run_copies(
            [
                pltpu.make_async_copy(
                    x_refs[i], x_buf.at[pl.ds(pl.multiple_of((core ^ i) * rows, rows), rows)], x_sem.at[i]
                )
                for i in range(len(chunks))
            ]
        )
        w_copies = []
        for j in range(slots):
            start = pl.multiple_of((hz ^ j) * width, width)
            w_copies.append(
                run_copies(
                    [
                        pltpu.make_async_copy(
                            w_refs[i].at[:, pl.ds(start, width)],
                            w_buf.at[j, :, pl.ds(i * width, width)],
                            w_sem.at[j, i],
                        )
                        for i in range(3)
                    ]
                )
            )
        for copy in x_copies:
            copy.wait()
        for j in range(slots):
            for copy in w_copies[j]:
                copy.wait()
            result = jnp.dot(x_buf[...], w_buf[j], preferred_element_type=F32).astype(BF16)
            for i in range(3):
                outs[j][i] = result[:, i * width : (i + 1) * width]

    return pl.pallas_call(
        kernel,
        out_shape=[jax.ShapeDtypeStruct((3, group, width), BF16)] * slots,
        in_specs=[SMEM] + [ANY] * (len(chunks) + 3),
        out_specs=[VMEM] * slots,
        scratch_shapes=[
            pltpu.VMEM((group, depth), BF16),
            pltpu.VMEM((slots, depth, 3 * width), BF16),
            pltpu.SemaphoreType.DMA((len(chunks),)),
            pltpu.SemaphoreType.DMA((slots, 3)),
        ],
        compiler_params=params(),
        cost_estimate=pl.CostEstimate(
            flops=2 * group * depth * 3 * width * slots,
            bytes_accessed=2 * (group * depth + depth * 3 * width * slots),
            transcendentals=0,
        ),
        name="project_a",
    )(place, *chunks, *weights)


def project_b(chunks, weights, place):
    rows, depth = chunks[0].shape
    total = rows * len(chunks)
    q_cols, kv_cols = weights[0].shape[1], weights[1].shape[1]

    def kernel(place_ref, *refs):
        x_refs = refs[: len(chunks)]
        w_refs = refs[len(chunks) : len(chunks) + 3]
        q_out, kv_out, tail_out, x_buf, q_buf, kv_buf, x_sem, w_sem = refs[len(chunks) + 3 :]
        t = place_ref[2]
        copies = run_copies(
            [
                pltpu.make_async_copy(
                    x_refs[i], x_buf.at[pl.ds(pl.multiple_of((t ^ i) * rows, rows), rows)], x_sem.at[i]
                )
                for i in range(len(chunks))
            ]
        )
        w_copies = run_copies(
            [
                pltpu.make_async_copy(w_refs[1], kv_buf.at[0], w_sem.at[1]),
                pltpu.make_async_copy(w_refs[2], kv_buf.at[1], w_sem.at[2]),
                pltpu.make_async_copy(w_refs[0], q_buf, w_sem.at[0]),
            ]
        )
        for copy in copies:
            copy.wait()
        for i in range(2):
            w_copies[i].wait()
            part = jnp.dot(x_buf[...], kv_buf[i], preferred_element_type=F32).astype(BF16)
            kv_out[i] = part
            tail_out[i] = part[total - WINDOW :]
        w_copies[2].wait()
        q_out[...] = jnp.dot(x_buf[...], q_buf[...], preferred_element_type=F32).astype(BF16)

    return pl.pallas_call(
        kernel,
        out_shape=[
            jax.ShapeDtypeStruct((total, q_cols), BF16),
            jax.ShapeDtypeStruct((2, total, kv_cols), BF16),
            jax.ShapeDtypeStruct((2, WINDOW, kv_cols), BF16),
        ],
        in_specs=[SMEM] + [ANY] * (len(chunks) + 3),
        out_specs=[VMEM] * 3,
        scratch_shapes=[
            pltpu.VMEM((total, depth), BF16),
            pltpu.VMEM((depth, q_cols), BF16),
            pltpu.VMEM((2, depth, kv_cols), BF16),
            pltpu.SemaphoreType.DMA((len(chunks),)),
            pltpu.SemaphoreType.DMA((3,)),
        ],
        compiler_params=params(),
        cost_estimate=pl.CostEstimate(
            flops=2 * total * depth * (q_cols + 2 * kv_cols),
            bytes_accessed=2 * (total * depth + depth * (q_cols + 2 * kv_cols)),
            transcendentals=0,
        ),
        name="project_b",
    )(place, *chunks, *weights)


def window_attention(query, pair, earlier, sinks, flag):
    total, q_cols = query.shape
    kv_cols = pair.shape[2]
    kv_heads = kv_cols // HEAD_DIM
    heads = q_cols // HEAD_DIM
    group_size = heads // kv_heads
    step = WINDOW
    blocks = total // step

    def kernel(flag_ref, sink_ref, q_ref, pair_ref, earlier_ref, out_ref, near):
        for i in range(2):
            near[i, :step] = earlier_ref[i]
            near[i, step:] = pair_ref[i]
        first = flag_ref[1] == 0
        rows_at = lax.broadcasted_iota(jnp.int32, (step, 2 * step), 0)
        cols_at = lax.broadcasted_iota(jnp.int32, (step, 2 * step), 1)
        distance = rows_at + step - cols_at
        band = (distance >= 0) & (distance < WINDOW)

        def one_block(i, carry):
            start = pl.multiple_of(i * step, step)
            allowed = band & jnp.logical_or(cols_at >= step, jnp.logical_not(first & (i == 0)))
            q_rows = q_ref[pl.ds(start, step), :]
            keys = near[0, pl.ds(start, 2 * step), :]
            values = near[1, pl.ds(start, 2 * step), :]
            for head in range(heads):
                g = head // group_size
                q_head = q_rows[:, head * HEAD_DIM : (head + 1) * HEAD_DIM]
                k_head = keys[:, g * HEAD_DIM : (g + 1) * HEAD_DIM]
                v_head = values[:, g * HEAD_DIM : (g + 1) * HEAD_DIM]
                scores = lax.dot_general(
                    q_head, k_head, (((1,), (1,)), ((), ())), preferred_element_type=F32
                ) * HEAD_DIM ** (-0.5)
                scores = jnp.where(allowed, scores, mask_fill)
                sink = sink_ref[head]
                top = jnp.maximum(jnp.max(scores, axis=1, keepdims=True), sink)
                weights = jnp.exp(scores - top)
                whole = jnp.sum(weights, axis=1, keepdims=True) + jnp.exp(sink - top)
                probs = (weights / whole).astype(BF16)
                result = jnp.dot(probs, v_head, preferred_element_type=F32)
                out_ref[pl.ds(start, step), head * HEAD_DIM : (head + 1) * HEAD_DIM] = result.astype(BF16)
            return carry

        lax.fori_loop(0, blocks, one_block, 0)

    return pl.pallas_call(
        kernel,
        out_shape=jax.ShapeDtypeStruct((total, q_cols), BF16),
        in_specs=[SMEM, SMEM, VMEM, VMEM, VMEM],
        out_specs=VMEM,
        scratch_shapes=[pltpu.VMEM((2, step + total, kv_cols), BF16)],
        compiler_params=params(),
        cost_estimate=pl.CostEstimate(
            flops=4 * total * 2 * step * heads * HEAD_DIM * 4,
            bytes_accessed=4 * total * q_cols,
            transcendentals=total * 2 * step * heads,
        ),
        name="window_attention",
    )(flag, sinks, query, pair, earlier)


def head_attention(own, other, kq, place, head_lambda, gain, blocks, per_block, chip_groups):
    slots = len(own[0])
    group, width = own[0][0].shape[1:]
    total = blocks * chip_groups * group
    span = math.gcd(per_block * chip_groups * group, 1024)
    half = span // 2 if span // 2 >= group else span
    own_flat = [own[k][j] for k in range(chip_groups) for j in range(slots)]
    other_flat = [side[k][j] for side in other for k in range(chip_groups) for j in range(slots)]
    n_own, n_other = len(own_flat), len(other_flat)

    def kernel(place_ref, lambda_ref, gain_ref, *refs):
        own_refs = refs[:n_own]
        other_refs = refs[n_own : n_own + n_other]
        outs = refs[n_own + n_other : n_own + n_other + slots]
        k_buf, v_buf, q_buf, o_buf, top, tot, acc, sem = refs[n_own + n_other + slots :]
        hz, l, t = place_ref[0], place_ref[1], place_ref[2]
        chip = t // 2

        def tile(j, side, k):
            return (((hz ^ j) * per_block + (l ^ side)) * chip_groups + (chip ^ k)) * group

        copies = []
        at = 0
        for k in range(chip_groups):
            for j in range(slots):
                ref = own_refs[k * slots + j]
                rows = pl.ds(pl.multiple_of(tile(j, 0, k), group), group)
                copies.append(pltpu.make_async_copy(ref.at[1], k_buf.at[rows], sem.at[at]))
                copies.append(pltpu.make_async_copy(ref.at[2], v_buf.at[rows], sem.at[at + 1]))
                at += 2
                if k == kq:
                    copies.append(pltpu.make_async_copy(ref.at[0], q_buf.at[j], sem.at[at]))
                    at += 1
        for side in range(per_block - 1):
            for k in range(chip_groups):
                for j in range(slots):
                    ref = other_refs[(side * chip_groups + k) * slots + j]
                    rows = pl.ds(pl.multiple_of(tile(j, side + 1, k), group), group)
                    copies.append(pltpu.make_async_copy(ref.at[0], k_buf.at[rows], sem.at[at]))
                    copies.append(pltpu.make_async_copy(ref.at[1], v_buf.at[rows], sem.at[at + 1]))
                    at += 2
        run_copies(copies)
        for copy in copies:
            copy.wait()
        lane = lax.broadcasted_iota(jnp.int32, (group, width), 1)

        def one_slot(j, carry):
            q_start = tile(j, 0, kq)
            query = q_buf[j] * jnp.asarray(HEAD_DIM ** (-0.5), BF16)
            zero = jnp.zeros_like(query)
            maps = (jnp.where(lane < HEAD_DIM, query, zero), jnp.where(lane >= HEAD_DIM, query, zero))

            def visit(start, size, opening):
                start = pl.multiple_of(start, span)
                keys = k_buf[pl.ds(start, size), :]
                values = v_buf[pl.ds(start, size), :]
                scores = [
                    lax.dot_general(m, keys, (((1,), (1,)), ((), ())), preferred_element_type=F32) for m in maps
                ]
                for i in range(2):
                    current = scores[i]
                    if opening:
                        row = lax.broadcasted_iota(jnp.int32, (group, size), 0) + (q_start - start)
                        col = lax.broadcasted_iota(jnp.int32, (group, size), 1)
                        current = jnp.where(row >= col, current, mask_fill)
                    peak = jnp.max(current, axis=1, keepdims=True)
                    if not opening:
                        before = top[i]
                        peak = jnp.maximum(before, peak)
                    weights = jnp.exp(current - peak)
                    added = jnp.sum(weights, axis=1, keepdims=True)
                    gained = jnp.dot(weights.astype(BF16), values, preferred_element_type=F32)
                    top[i] = peak
                    if opening:
                        tot[i] = added
                        acc[i] = gained
                    else:
                        shrink = jnp.exp(before - peak)
                        tot[i] = tot[i] * shrink + added
                        acc[i] = acc[i] * shrink + gained

            full = q_start // span
            inside = q_start - full * span
            if half < span:

                @pl.when(inside + group <= half)
                def _():
                    visit(full * span, half, True)

                @pl.when(inside + group > half)
                def _():
                    visit(full * span, span, True)

            else:
                visit(full * span, span, True)

            def one_span(n, inner):
                visit(n * span, span, False)
                return inner

            lax.fori_loop(0, full, one_span, 0)
            lam = lambda_ref[hz]
            diff = acc[0] / tot[0] - lam * (acc[1] / tot[1])
            square = jnp.mean(diff * diff, axis=1, keepdims=True)
            o_buf[j] = (diff * lax.rsqrt(square + norm_eps) * gain_ref[...] * head_scale).astype(BF16)
            return carry

        lax.fori_loop(0, slots, one_slot, 0)
        for j in range(slots):
            outs[j][...] = o_buf[j]

    flops = 2 * slots * group * total * 2 * (256 + 256)
    return pl.pallas_call(
        kernel,
        out_shape=[jax.ShapeDtypeStruct((group, width), BF16)] * slots,
        in_specs=[SMEM, SMEM, VMEM] + [ANY] * (n_own + n_other),
        out_specs=[VMEM] * slots,
        scratch_shapes=[
            pltpu.VMEM((total, width), BF16),
            pltpu.VMEM((total, width), BF16),
            pltpu.VMEM((slots, group, width), BF16),
            pltpu.VMEM((slots, group, width), BF16),
            pltpu.VMEM((2, group, 1), F32),
            pltpu.VMEM((2, group, 1), F32),
            pltpu.VMEM((2, group, width), F32),
            pltpu.SemaphoreType.DMA((2 * (n_own + n_other) + slots,)),
        ],
        compiler_params=params(),
        cost_estimate=pl.CostEstimate(
            flops=flops, bytes_accessed=4 * total * width, transcendentals=slots * group * total
        ),
        name="head_attention",
    )(place, head_lambda, gain, *own_flat, *other_flat)


def project_out(a_parts, b_rows, a_weight, b_weight, place, k):
    slots = len(a_parts)
    group, width = a_parts[0].shape
    rows = group // 2
    b_cols, columns = b_weight.shape
    a_cols = a_weight.shape[0]
    tile = math.gcd(columns, 1024)

    def kernel(place_ref, *refs):
        a_refs = refs[:slots]
        b_ref, aw_ref, bw_ref, mine_ref, other_ref, lhs, out_buf, sem = refs[slots:]
        hz, t = place_ref[0], place_ref[2]

        @pl.when(pl.program_id(0) == 0)
        def _():
            start = pl.multiple_of(((t // 2) ^ k) * group, group)
            copies = [
                pltpu.make_async_copy(
                    a_refs[j], lhs.at[:, pl.ds(pl.multiple_of((hz ^ j) * width, width), width)], sem.at[j]
                )
                for j in range(slots)
            ]
            copies.append(
                pltpu.make_async_copy(
                    b_ref.at[pl.ds(start, group)], lhs.at[:, a_cols : a_cols + b_cols], sem.at[slots]
                )
            )
            run_copies(copies)
            for copy in copies:
                copy.wait()

        out_buf[...] = jnp.dot(lhs[:, :a_cols], aw_ref[...], preferred_element_type=F32) + jnp.dot(
            lhs[:, a_cols:], bw_ref[...], preferred_element_type=F32
        )
        core = t % 2
        mine_ref[...] = out_buf[pl.ds(pl.multiple_of(core * rows, rows), rows), :].astype(BF16)
        other_ref[...] = out_buf[pl.ds(pl.multiple_of((1 - core) * rows, rows), rows), :].astype(BF16)

    return pl.pallas_call(
        kernel,
        grid=(columns // tile,),
        out_shape=[jax.ShapeDtypeStruct((rows, columns), BF16)] * 2,
        in_specs=[SMEM]
        + [ANY] * (slots + 1)
        + [pl.BlockSpec((a_cols, tile), lambda n: (0, n)), pl.BlockSpec((b_cols, tile), lambda n: (0, n))],
        out_specs=[pl.BlockSpec((rows, tile), lambda n: (0, n))] * 2,
        scratch_shapes=[
            pltpu.VMEM((group, a_cols + b_cols), BF16),
            pltpu.VMEM((group, tile), F32),
            pltpu.SemaphoreType.DMA((slots + 1,)),
        ],
        compiler_params=params(),
        cost_estimate=pl.CostEstimate(
            flops=2 * group * (a_cols + b_cols) * columns,
            bytes_accessed=2 * (a_cols + b_cols) * columns,
            transcendentals=0,
        ),
        name="project_out",
    )(place, *a_parts, b_rows, a_weight, b_weight)


def shards(
    inputs,
    a_query_w,
    a_key_w,
    a_value_w,
    b_query_w,
    b_key_w,
    b_value_w,
    head_lambda,
    head_gain,
    sink_logit,
    a_out_w,
    b_out_w,
):
    sp, tp = lax.axis_size("sp"), lax.axis_size("tp")
    chips = tp // 2
    slots = head_lambda.shape[0]
    per_block = sp // slots
    s, t = lax.axis_index("sp"), lax.axis_index("tp")
    place = jnp.stack([s // per_block, s % per_block, t]).astype(jnp.int32)
    flag = jnp.stack([t, s]).astype(jnp.int32)

    chunks = [inputs, None] + [None] * (tp - 2)
    for k in range(1, chips):
        chunks[2 * k] = swap(inputs, "tp", 2 * k)
    for k in range(chips):
        chunks[2 * k + 1] = swap(chunks[2 * k], "tp", 1)

    own, other = [], [[] for _ in range(per_block - 1)]
    for k in range(chips):
        made = project_a(chunks[2 * k : 2 * k + 2], (a_query_w, a_key_w, a_value_w), place, slots)
        got = [made[0]] + [swap(made[j], "sp", j * per_block) for j in range(1, slots)]
        own.append(got)
        for side in range(1, per_block):
            other[side - 1].append([swap(part[1:], "sp", side) for part in got])

    b_query, b_pair, b_tail = project_b(chunks, (b_query_w, b_key_w, b_value_w), place)
    earlier = lax.ppermute(b_tail, "sp", [(i, i + 1) for i in range(sp - 1)])
    b_heads = window_attention(b_query, b_pair, earlier, sink_logit, flag)

    gain = head_gain.reshape(1, VALUE_DIM)
    received = []
    mine_own = None
    for k in list(range(1, chips)) + [0]:
        parts = head_attention(own, other, k, place, head_lambda, gain, sp, per_block, chips)
        parts = [parts[0]] + [swap(parts[j], "sp", j * per_block) for j in range(1, slots)]
        mine, sibling = project_out(parts, b_heads, a_out_w, b_out_w, place, k)
        handed = swap(sibling, "tp", 1)
        if k:
            joined = (mine.astype(F32) + handed.astype(F32)).astype(BF16)
            received.append(swap(joined, "tp", 2 * k))
        else:
            mine_own = mine.astype(F32) + handed.astype(F32)
    for part in received:
        mine_own = mine_own + part.astype(F32)
    return mine_own.astype(BF16)


def solution(mesh):
    return jax.shard_map(
        shards,
        mesh=mesh,
        in_specs=(
            P(("sp", "tp"), None),
            P(None, "tp"),
            P(None, "tp"),
            P(None, "tp"),
            P(None, "tp"),
            P(None, "tp"),
            P(None, "tp"),
            P("tp"),
            P(),
            P("tp"),
            P("tp", None),
            P("tp", None),
        ),
        out_specs=P(("sp", "tp"), None),
        check_vma=False,
    )
```
